32 devices in a mesh: sp: 8 (over z, y), tp: 4 (over x, core).
Axes of the slice: x: 2, y: 2, z: 4, core: 2. Of those that a mesh axis runs over, the one named last changes fastest.
Arguments:
- inputs: bfloat16 [8192, 2048], P('sp'), may hold values from -6 to 6
- norm_gain: float32 [3, 2048], replicated, may hold values from 0.1 to 1.9
- query_weight: bfloat16 [3, 2048, 1024], P(None, 'sp', 'tp'), may hold values from -64 to 64
- key_weight: bfloat16 [3, 2048, 512], P(None, 'sp', 'tp'), may hold values from -4 to 4
- value_weight: bfloat16 [3, 2048, 512], P(None, 'sp', 'tp'), may hold values from -0.125 to 0.125
- output_weight: bfloat16 [3, 2048, 1024], P(None, 'sp', 'tp'), may hold values from -0.1875 to 0.1875
- sink_logit: float32 [3, 16], P(None, 'tp'), may hold values from 2 to 7
- final_gain: float32 [2048], replicated, may hold values from 0.1 to 1.9
Outputs:
- result: float32 [8192, 2048], P(('sp', 'tp'))
The draws below stay inside these ranges and needn't reach their ends.
All inputs are finite; a program needn't handle non-finite values.
Results may differ from the reference program's by a relative error of at most 0.015.
Values may be sent and summed in bfloat16 or wider, within the bound.
No kernel may reach another device: no remote copies, remote signals or barrier semaphores. Data moves between devices by JAX's collectives and lax.ppermute only.
A program may use at most 64 MiB of HBM per device.

```python
import jax
import jax.numpy as jnp
from jax import lax

D = 2048
HEADS = 16
KV_HEADS = 8
HEAD_DIM = 64
WINDOW = 128
LAYERS = 3
TOK_DEV = 1024
SEQ = 8192


def shared_keys(key):
    base_key = jax.random.fold_in(key, 7)
    shape = (LAYERS, D, KV_HEADS * HEAD_DIM)
    return jnp.clip(jax.random.normal(base_key, shape, jnp.float32), -4.0, 4.0)


def draw_key_weight(key, part):
    return shared_keys(key).astype(jnp.bfloat16)


def draw_query_weight(key, part):
    base_key = jax.random.fold_in(key, 13)
    drawn = jax.random.normal(base_key, (LAYERS, D, HEADS * HEAD_DIM), jnp.float32)
    return jnp.clip(drawn, -4.0, 4.0).astype(jnp.bfloat16)


def level_of(key, dims, shards, smallest, high):
    loudness = 1.0
    for position, parts in shards:
        draws = jax.random.uniform(jax.random.fold_in(jax.random.fold_in(key, 6), position), (parts,), jnp.float32, smallest / len(shards), high / len(shards))
        loudness = loudness * jnp.repeat(jnp.exp(draws), dims[position] // parts).reshape((-1,) + (1,) * (len(dims) - 1 - position))
    return loudness


def bell_draw(own_key, extent, deviation, bound, cuts=(), kind=jnp.bfloat16):
    values = jax.random.normal(own_key, extent, jnp.float32) * deviation
    if len(cuts) > 0:
        values = level_of(own_key, extent, cuts, -0.22, 0.18) * values
    return jnp.clip(values, min=-bound, max=bound).astype(kind)


def setup_inputs(seed: int = 0) -> dict:
    streams_of = jax.random.split(jax.random.key(seed), 9)
    inputs = bell_draw(streams_of[0], (SEQ, D), 1.0, 6.0, ((0, 8),))
    norm_gain = jnp.clip(1.0 + 0.18 * jax.random.normal(streams_of[1], (LAYERS, D), jnp.float32), 0.1, 1.9)
    query_weight = draw_query_weight(jax.random.fold_in(streams_of[8], 71), 0)
    key_weight = draw_key_weight(jax.random.fold_in(streams_of[8], 71), 0)
    value_weight = bell_draw(streams_of[4], (LAYERS, D, KV_HEADS * HEAD_DIM), D ** -0.5, 0.125, ((1, 8), (2, 4)))
    output_weight = bell_draw(streams_of[5], (LAYERS, D, HEADS * HEAD_DIM), (HEADS * HEAD_DIM) ** -0.5, 0.1875, ((1, 8), (2, 4)))
    sink_logit = jnp.clip(2.0 + 5.0 * jax.random.uniform(streams_of[6], (LAYERS, HEADS), jnp.float32) ** level_of(streams_of[6], (LAYERS, HEADS), ((1, 4),), -0.2, 0.2), 2.0, 7.0)
    final_gain = jnp.clip(1.0 + 0.18 * jax.random.normal(streams_of[7], (D,), jnp.float32), 0.1, 1.9)
    return {"inputs": inputs, "norm_gain": norm_gain, "query_weight": query_weight, "key_weight": key_weight, "value_weight": value_weight, "output_weight": output_weight, "sink_logit": sink_logit, "final_gain": final_gain}


EPS = 1e-06

def norm_rows(values, gain):
    wide_values = values.astype(jnp.float32)
    inv_root = lax.rsqrt(lax.optimization_barrier(jnp.mean(wide_values * wide_values, axis=-1, keepdims=True)) + EPS)
    return wide_values * inv_root * gain

def rotate(values, places):
    half_dim = values.shape[-1] // 2
    inverse = 10000.0 ** (-jnp.arange(half_dim).astype(jnp.float32) / half_dim)
    angles = places[:, None] * inverse[None, :]
    cosine_table = jnp.cos(angles)[:, None, :]
    sine_table = jnp.sin(angles)[:, None, :]
    front_half = values[..., :half_dim]
    back_half = values[..., half_dim:]
    return jnp.concatenate([front_half * cosine_table - back_half * sine_table, back_half * cosine_table + front_half * sine_table], axis=-1)

def attend(queries, key_rows, value_rows, sink_row, allowed):
    scores = jnp.einsum('qkgd,skd->kgqs', queries.astype(jnp.float32), key_rows.astype(jnp.float32)) * queries.shape[-1] ** (-0.5)
    scores = jnp.where(allowed[None, None], scores, -jnp.inf)
    sink_col = sink_row[:, :, None]
    largest = jnp.maximum(lax.optimization_barrier(jnp.max(scores, axis=-1)), sink_col)
    powers = jnp.exp(scores - largest[..., None])
    denominator = lax.optimization_barrier(jnp.sum(powers, axis=-1)) + jnp.exp(sink_col - largest)
    weights = (powers / denominator[..., None]).astype(jnp.bfloat16)
    blended = jnp.einsum('kgqs,skd->qkgd', weights.astype(jnp.float32), value_rows.astype(jnp.float32))
    return blended.astype(jnp.bfloat16)

def reference(inputs, norm_gain, query_weight, key_weight, value_weight, output_weight, sink_logit, final_gain):
    seq_total = inputs.shape[0]
    blocks = seq_total // TOK_DEV
    per_group = HEADS // KV_HEADS
    places = jnp.arange(seq_total).astype(jnp.float32)
    current = inputs
    for layer in range(LAYERS):
        normed = norm_rows(current, norm_gain[layer]).astype(jnp.bfloat16)
        query_raw = jnp.dot(normed, query_weight[layer], preferred_element_type=jnp.float32) * float(D) ** (-0.5)
        key_raw = jnp.dot(normed, key_weight[layer], preferred_element_type=jnp.float32) * float(D) ** (-0.5)
        value_raw = jnp.dot(normed, value_weight[layer], preferred_element_type=jnp.float32)
        queries = rotate(query_raw.reshape(seq_total, HEADS, HEAD_DIM), places).astype(jnp.bfloat16)
        queries = queries.reshape(seq_total, KV_HEADS, per_group, HEAD_DIM)
        key_rot = rotate(key_raw.reshape(seq_total, KV_HEADS, HEAD_DIM), places).astype(jnp.bfloat16)
        value_all = value_raw.astype(jnp.bfloat16).reshape(seq_total, KV_HEADS, HEAD_DIM)
        padding = ((WINDOW, WINDOW), (0, 0), (0, 0))
        pad_keys = jnp.pad(key_rot, padding)
        pad_values = jnp.pad(value_all, padding)
        sink_row = sink_logit[layer].reshape(KV_HEADS, per_group)

        def one_block(block_index):
            first_row = block_index * TOK_DEV
            block_queries = lax.dynamic_slice_in_dim(queries, first_row, TOK_DEV, 0)
            block_keys = lax.dynamic_slice_in_dim(pad_keys, first_row, TOK_DEV + 2 * WINDOW, 0)
            block_values = lax.dynamic_slice_in_dim(pad_values, first_row, TOK_DEV + 2 * WINDOW, 0)
            query_pos = first_row + jnp.arange(TOK_DEV, dtype=jnp.int32)
            key_pos = first_row - WINDOW + jnp.arange(TOK_DEV + 2 * WINDOW, dtype=jnp.int32)
            allowed = (jnp.abs(key_pos[None, :] - query_pos[:, None]) <= WINDOW) & (key_pos[None, :] >= 0) & (key_pos[None, :] < seq_total)
            return attend(block_queries, block_keys, block_values, sink_row, allowed)
        attended = lax.map(one_block, jnp.arange(blocks, dtype=jnp.int32)).reshape(seq_total, HEADS * HEAD_DIM)
        current = jnp.dot(attended, output_weight[layer].T, preferred_element_type=jnp.float32).astype(jnp.bfloat16)
    return norm_rows(current, final_gain)
```

```python
import jax
import jax.numpy as jnp
from jax import lax
from jax.sharding import PartitionSpec as P

HEAD_DIM = 64
WINDOW = 128
EPS = 1e-06
BOTH = ("sp", "tp")
QUERY_BLOCK = 256


def norm_rows(values, gain):
    wide_values = values.astype(jnp.float32)
    inv_root = lax.rsqrt(jnp.mean(wide_values * wide_values, axis=-1, keepdims=True) + EPS)
    return wide_values * inv_root * gain


def rotate(values, cosine_table, sine_table):
    half_dim = values.shape[-1] // 2
    front_half = values[..., :half_dim]
    back_half = values[..., half_dim:]
    return jnp.concatenate(
        [
            front_half * cosine_table - back_half * sine_table,
            back_half * cosine_table + front_half * sine_table,
        ],
        axis=-1,
    )


def attend(queries, key_rows, value_rows, sink_row, allowed):
    scores = jnp.einsum(
        "qkgd,skd->kgqs", queries, key_rows, preferred_element_type=jnp.float32
    ) * queries.shape[-1] ** (-0.5)
    scores = jnp.where(allowed[None, None], scores, -jnp.inf)
    sink_col = sink_row[:, :, None]
    largest = jnp.maximum(jnp.max(scores, axis=-1), sink_col)
    powers = jnp.exp(scores - largest[..., None])
    denominator = jnp.sum(powers, axis=-1) + jnp.exp(sink_col - largest)
    weights = (powers / denominator[..., None]).astype(jnp.bfloat16)
    blended = jnp.einsum("kgqs,skd->qkgd", weights, value_rows, preferred_element_type=jnp.float32)
    return blended.astype(jnp.bfloat16)


def make_shards(sp_size, tp_size):
    cores = 2 if tp_size % 2 == 0 else 1
    xs = tp_size // cores
    ys = 1
    while ys * ys * 4 <= sp_size and sp_size % (ys * 2) == 0:
        ys *= 2
    if sp_size % ys:
        ys = 1
    zs = sp_size // ys

    def pairs_of(move):
        pairs = []
        for z in range(zs):
            for y in range(ys):
                for x in range(xs):
                    for c in range(cores):
                        target = move(z, y, x, c)
                        if target is not None:
                            tz, ty, tx, tc = target
                            source = ((z * ys + y) * xs + x) * cores + c
                            pairs.append((source, ((tz * ys + ty) * xs + tx) * cores + tc))
        return pairs

    down_z = pairs_of(lambda z, y, x, c: ((z - 1) % zs, y, x, c))
    down_y = pairs_of(lambda z, y, x, c: (z, (y - 1) % ys, x, c))
    down_x = pairs_of(lambda z, y, x, c: (z, y, (x - 1) % xs, c))
    other_core = pairs_of(lambda z, y, x, c: (z, y, x, (c + 1) % cores))
    spans = sp_size * xs
    forward = [
        (s * cores + c, (s + 1) * cores + c) for s in range(spans - 1) for c in range(cores)
    ]
    backward = [(target, source) for source, target in forward]

    def ring(block, pairs, count):
        parts = [block]
        for _ in range(count - 1):
            parts.append(lax.ppermute(parts[-1], BOTH, pairs))
        return jnp.stack(parts)

    def shards(
        inputs, norm_gain, query_weight, key_weight, value_weight, output_weight, sink_logit,
        final_gain,
    ):
        layers, rows, q_cols = query_weight.shape
        kv_cols = key_weight.shape[2]
        features = inputs.shape[1]
        span = inputs.shape[0] // xs
        share = span // cores
        groups = xs * kv_cols // HEAD_DIM
        heads = xs * q_cols // HEAD_DIM
        per_group = heads // groups
        sp_id = lax.axis_index("sp")
        tp_id = lax.axis_index("tp")
        z_id, y_id = sp_id // ys, sp_id % ys
        x_id, core_id = tp_id // cores, tp_id % cores
        seq_total = inputs.shape[0] * sp_size
        offset = (sp_id * xs + x_id) * span

        def to_local(values):
            parts = []
            for j in range(ys):
                for i in range(zs):
                    block = ((z_id + i) % zs) * ys + (y_id + j) % ys
                    parts.append(lax.dynamic_slice_in_dim(values, block * rows, rows, axis=-1))
            return jnp.concatenate(parts, axis=-1)

        def to_global(values):
            parts = []
            for zb in range(zs):
                for yb in range(ys):
                    place = ((yb - y_id) % ys) * zs + (zb - z_id) % zs
                    parts.append(lax.dynamic_slice_in_dim(values, place * rows, rows, axis=-1))
            return jnp.concatenate(parts, axis=-1)

        whole = []
        for layer in range(layers):
            first = jnp.concatenate([query_weight[layer], key_weight[layer]], axis=1)
            second = jnp.concatenate([output_weight[layer], value_weight[layer]], axis=1)
            both = ring(jnp.stack([first, second]), down_z, zs)
            first = ring(both[:, 0], down_y, ys)
            first = ring(first, down_x, xs)
            second = ring(both[:, 1], down_x, xs)
            second = jnp.swapaxes(ring(second, down_y, ys), 0, 1)
            whole.append(
                (first.reshape(xs, features, -1), second.reshape(xs, features, -1))
            )
        sinks = ring(sink_logit, down_x, xs)

        query_pos = offset + jnp.arange(span, dtype=jnp.int32)
        places = query_pos.astype(jnp.float32)
        half_dim = HEAD_DIM // 2
        inverse = 10000.0 ** (-jnp.arange(half_dim).astype(jnp.float32) / half_dim)
        angles = places[:, None] * inverse[None, :]
        cosine_table = jnp.cos(angles)[:, None, :]
        sine_table = jnp.sin(angles)[:, None, :]
        gains = to_local(norm_gain)
        current = to_local(lax.dynamic_slice_in_dim(inputs, x_id * span, span, axis=0))
        scale = float(features) ** (-0.5)
        block = QUERY_BLOCK if span % QUERY_BLOCK == 0 else span
        final_rows = None
        for layer in range(layers):
            first, second = whole[layer]
            normed = norm_rows(current, gains[layer]).astype(jnp.bfloat16)

            def times(weight):
                return jnp.concatenate(
                    [
                        jnp.dot(normed, weight[r], preferred_element_type=jnp.float32)
                        for r in range(xs)
                    ],
                    axis=1,
                )

            key_raw = times(first[:, :, q_cols:])
            value_raw = times(second[:, :, q_cols:])
            key_rot = rotate(
                (key_raw * scale).reshape(span, groups, HEAD_DIM), cosine_table, sine_table
            ).astype(jnp.bfloat16)
            packed = jnp.stack(
                [
                    key_rot.reshape(span, xs, kv_cols),
                    value_raw.astype(jnp.bfloat16).reshape(span, xs, kv_cols),
                ],
                axis=1,
            )
            low = jnp.roll(lax.ppermute(packed[span - WINDOW :], BOTH, forward), -1, axis=2)
            high = jnp.roll(lax.ppermute(packed[:WINDOW], BOTH, backward), 1, axis=2)
            query_raw = times(first[:, :, :q_cols])
            queries = rotate(
                (query_raw * scale).reshape(span, heads, HEAD_DIM), cosine_table, sine_table
            ).astype(jnp.bfloat16)
            queries = queries.reshape(span, groups, per_group, HEAD_DIM)
            extended = jnp.concatenate([low, packed, high], axis=0)
            key_rows = extended[:, 0].reshape(-1, groups, HEAD_DIM)
            value_rows = extended[:, 1].reshape(-1, groups, HEAD_DIM)
            sink_row = sinks[:, layer].reshape(groups, per_group)
            pieces = []
            for start in range(0, span, block):
                stop = start + block + 2 * WINDOW
                key_pos = offset - WINDOW + jnp.arange(start, stop, dtype=jnp.int32)
                own_pos = query_pos[start : start + block]
                allowed = (
                    (jnp.abs(key_pos[None, :] - own_pos[:, None]) <= WINDOW)
                    & (key_pos[None, :] >= 0)
                    & (key_pos[None, :] < seq_total)
                )
                pieces.append(
                    attend(
                        queries[start : start + block],
                        key_rows[start:stop],
                        value_rows[start:stop],
                        sink_row,
                        allowed,
                    )
                )
            attended = jnp.concatenate(pieces, axis=0).reshape(span, xs, q_cols)

            def project(rows_of):
                total = 0.0
                for r in range(xs):
                    total = total + lax.dot_general(
                        rows_of[:, r],
                        second[r, :, :q_cols],
                        (((1,), (1,)), ((), ())),
                        preferred_element_type=jnp.float32,
                    )
                return total

            if layer < layers - 1:
                total = project(attended)
                if cores > 1:
                    total = total + lax.ppermute(
                        total.astype(jnp.bfloat16), BOTH, other_core
                    ).astype(jnp.float32)
                current = total.astype(jnp.bfloat16)
            else:
                kept = lax.dynamic_slice_in_dim(attended, core_id * share, share, axis=0)
                total = project(kept)
                if cores > 1:
                    away = (1 - core_id) * share
                    sent = lax.dynamic_slice_in_dim(attended, away, share, axis=0)
                    sent = project(sent).astype(jnp.bfloat16)
                    total = total + lax.ppermute(sent, BOTH, other_core).astype(jnp.float32)
                final_rows = total.astype(jnp.bfloat16)
        return norm_rows(to_global(final_rows), final_gain)

    return shards


def solution(mesh):
    in_specs = (
        P("sp", None),
        P(),
        P(None, "sp", "tp"),
        P(None, "sp", "tp"),
        P(None, "sp", "tp"),
        P(None, "sp", "tp"),
        P(None, "tp"),
        P(),
    )
    out_specs = P(("sp", "tp"), None)
    shards = make_shards(mesh.shape["sp"], mesh.shape["tp"])
    return jax.shard_map(shards, mesh=mesh, in_specs=in_specs, out_specs=out_specs, check_vma=False)
```

```python
import jax
import jax.numpy as jnp
from jax import lax
from jax.sharding import PartitionSpec as P

HEAD_DIM = 64
WINDOW = 128
EPS = 1e-06
BOTH = ("sp", "tp")
QUERY_BLOCK = 256


def norm_rows(values, gain):
    wide_values = values.astype(jnp.float32)
    inv_root = lax.rsqrt(jnp.mean(wide_values * wide_values, axis=-1, keepdims=True) + EPS)
    return wide_values * inv_root * gain


def rotate(values, cosine_table, sine_table):
    half_dim = values.shape[-1] // 2
    front_half = values[..., :half_dim]
    back_half = values[..., half_dim:]
    return jnp.concatenate(
        [
            front_half * cosine_table - back_half * sine_table,
            back_half * cosine_table + front_half * sine_table,
        ],
        axis=-1,
    )


def attend(queries, key_rows, value_rows, sink_row, allowed):
    scores = jnp.einsum(
        "qkgd,skd->kgqs", queries, key_rows, preferred_element_type=jnp.float32
    ) * queries.shape[-1] ** (-0.5)
    scores = jnp.where(allowed[None, None], scores, -jnp.inf)
    sink_col = sink_row[:, :, None]
    largest = jnp.maximum(jnp.max(scores, axis=-1), sink_col)
    powers = jnp.exp(scores - largest[..., None])
    denominator = jnp.sum(powers, axis=-1) + jnp.exp(sink_col - largest)
    weights = (powers / denominator[..., None]).astype(jnp.bfloat16)
    blended = jnp.einsum("kgqs,skd->qkgd", weights, value_rows, preferred_element_type=jnp.float32)
    return blended.astype(jnp.bfloat16)


def make_shards(sp_size, tp_size):
    cores = 2 if tp_size % 2 == 0 else 1
    xs = tp_size // cores
    ys = 1
    while ys * ys * 4 <= sp_size and sp_size % (ys * 2) == 0:
        ys *= 2
    if sp_size % ys:
        ys = 1
    zs = sp_size // ys

    def pairs_of(move):
        pairs = []
        for z in range(zs):
            for y in range(ys):
                for x in range(xs):
                    for c in range(cores):
                        target = move(z, y, x, c)
                        if target is not None:
                            tz, ty, tx, tc = target
                            source = ((z * ys + y) * xs + x) * cores + c
                            pairs.append((source, ((tz * ys + ty) * xs + tx) * cores + tc))
        return pairs

    down_z = pairs_of(lambda z, y, x, c: ((z - 1) % zs, y, x, c))
    down_y = pairs_of(lambda z, y, x, c: (z, (y - 1) % ys, x, c))
    down_x = pairs_of(lambda z, y, x, c: (z, y, (x - 1) % xs, c))
    other_core = pairs_of(lambda z, y, x, c: (z, y, x, (c + 1) % cores))
    spans = sp_size * xs
    forward = [
        (s * cores + c, (s + 1) * cores + c) for s in range(spans - 1) for c in range(cores)
    ]
    backward = [(target, source) for source, target in forward]

    def ring(block, pairs, count):
        parts = [block]
        for _ in range(count - 1):
            parts.append(lax.ppermute(parts[-1], BOTH, pairs))
        return jnp.stack(parts)

    def shards(
        inputs, norm_gain, query_weight, key_weight, value_weight, output_weight, sink_logit,
        final_gain,
    ):
        layers, rows, q_cols = query_weight.shape
        kv_cols = key_weight.shape[2]
        features = inputs.shape[1]
        span = inputs.shape[0] // xs
        share = span // cores
        groups = xs * kv_cols // HEAD_DIM
        heads = xs * q_cols // HEAD_DIM
        per_group = heads // groups
        sp_id = lax.axis_index("sp")
        tp_id = lax.axis_index("tp")
        z_id, y_id = sp_id // ys, sp_id % ys
        x_id, core_id = tp_id // cores, tp_id % cores
        seq_total = inputs.shape[0] * sp_size
        offset = (sp_id * xs + x_id) * span

        def to_local(values):
            parts = []
            for j in range(ys):
                for i in range(zs):
                    block = ((z_id + i) % zs) * ys + (y_id + j) % ys
                    parts.append(lax.dynamic_slice_in_dim(values, block * rows, rows, axis=-1))
            return jnp.concatenate(parts, axis=-1)

        def to_global(values):
            parts = []
            for zb in range(zs):
                for yb in range(ys):
                    place = ((yb - y_id) % ys) * zs + (zb - z_id) % zs
                    parts.append(lax.dynamic_slice_in_dim(values, place * rows, rows, axis=-1))
            return jnp.concatenate(parts, axis=-1)

        def halves(layer):
            first = jnp.concatenate([query_weight[layer], key_weight[layer]], axis=1)
            second = jnp.concatenate([output_weight[layer], value_weight[layer]], axis=1)
            return jnp.stack([first, second])

        early = ring(halves(0), down_z, zs)
        late = ring(jnp.stack([halves(layer) for layer in range(1, layers)]), down_z, zs)
        whole = []
        for layer in range(layers):
            both = early if layer == 0 else late[:, layer - 1]
            first = ring(both[:, 0], down_y, ys)
            second = ring(both[:, 1], down_x, xs)
            first = ring(first, down_x, xs)
            second = jnp.swapaxes(ring(second, down_y, ys), 0, 1)
            whole.append(
                (first.reshape(xs, features, -1), second.reshape(xs, features, -1))
            )
        sinks = ring(sink_logit, down_x, xs)

        query_pos = offset + jnp.arange(span, dtype=jnp.int32)
        places = query_pos.astype(jnp.float32)
        half_dim = HEAD_DIM // 2
        inverse = 10000.0 ** (-jnp.arange(half_dim).astype(jnp.float32) / half_dim)
        angles = places[:, None] * inverse[None, :]
        cosine_table = jnp.cos(angles)[:, None, :]
        sine_table = jnp.sin(angles)[:, None, :]
        gains = to_local(norm_gain)
        current = to_local(lax.dynamic_slice_in_dim(inputs, x_id * span, span, axis=0))
        scale = float(features) ** (-0.5)
        block = QUERY_BLOCK if span % QUERY_BLOCK == 0 else span
        final_rows = None
        for layer in range(layers):
            first, second = whole[layer]
            normed = norm_rows(current, gains[layer]).astype(jnp.bfloat16)

            def times(weight):
                return jnp.concatenate(
                    [
                        jnp.dot(normed, weight[r], preferred_element_type=jnp.float32)
                        for r in range(xs)
                    ],
                    axis=1,
                )

            key_raw = times(first[:, :, q_cols:])
            value_raw = times(second[:, :, q_cols:])
            key_rot = rotate(
                (key_raw * scale).reshape(span, groups, HEAD_DIM), cosine_table, sine_table
            ).astype(jnp.bfloat16)
            packed = jnp.stack(
                [
                    key_rot.reshape(span, xs, kv_cols),
                    value_raw.astype(jnp.bfloat16).reshape(span, xs, kv_cols),
                ],
                axis=1,
            )
            low = lax.ppermute(packed[span - WINDOW :], BOTH, forward)
            high = lax.ppermute(packed[:WINDOW], BOTH, backward)
            low = jnp.roll(low, -1, axis=2)
            high = jnp.roll(high, 1, axis=2)
            query_raw = times(first[:, :, :q_cols])
            queries = rotate(
                (query_raw * scale).reshape(span, heads, HEAD_DIM), cosine_table, sine_table
            ).astype(jnp.bfloat16)
            queries = queries.reshape(span, groups, per_group, HEAD_DIM)
            extended = jnp.concatenate([low, packed, high], axis=0)
            key_rows = extended[:, 0].reshape(-1, groups, HEAD_DIM)
            value_rows = extended[:, 1].reshape(-1, groups, HEAD_DIM)
            sink_row = sinks[:, layer].reshape(groups, per_group)
            pieces = []
            for start in range(0, span, block):
                stop = start + block + 2 * WINDOW
                key_pos = offset - WINDOW + jnp.arange(start, stop, dtype=jnp.int32)
                own_pos = query_pos[start : start + block]
                allowed = (
                    (jnp.abs(key_pos[None, :] - own_pos[:, None]) <= WINDOW)
                    & (key_pos[None, :] >= 0)
                    & (key_pos[None, :] < seq_total)
                )
                pieces.append(
                    attend(
                        queries[start : start + block],
                        key_rows[start:stop],
                        value_rows[start:stop],
                        sink_row,
                        allowed,
                    )
                )
            attended = jnp.concatenate(pieces, axis=0).reshape(span, xs, q_cols)

            def project(rows_of):
                total = 0.0
                for r in range(xs):
                    total = total + lax.dot_general(
                        rows_of[:, r],
                        second[r, :, :q_cols],
                        (((1,), (1,)), ((), ())),
                        preferred_element_type=jnp.float32,
                    )
                return total

            if layer < layers - 1:
                total = project(attended)
                if cores > 1:
                    other = lax.ppermute(total.astype(jnp.bfloat16), BOTH, other_core)
                    total = total + other.astype(jnp.float32)
                current = total.astype(jnp.bfloat16)
            else:
                kept = lax.dynamic_slice_in_dim(attended, core_id * share, share, axis=0)
                total = project(kept)
                if cores > 1:
                    away = (1 - core_id) * share
                    sent = lax.dynamic_slice_in_dim(attended, away, share, axis=0)
                    sent = project(sent).astype(jnp.bfloat16)
                    total = total + lax.ppermute(sent, BOTH, other_core).astype(jnp.float32)
                final_rows = total.astype(jnp.bfloat16)
        return norm_rows(to_global(final_rows), final_gain)

    return shards


def solution(mesh):
    in_specs = (
        P("sp", None),
        P(),
        P(None, "sp", "tp"),
        P(None, "sp", "tp"),
        P(None, "sp", "tp"),
        P(None, "sp", "tp"),
        P(None, "tp"),
        P(),
    )
    out_specs = P(("sp", "tp"), None)
    sp_size, tp_size = mesh.shape["sp"], mesh.shape["tp"]
    shards = make_shards(sp_size, tp_size)

    return jax.shard_map(shards, mesh=mesh, in_specs=in_specs, out_specs=out_specs, check_vma=False)
```
